32 devices in a mesh: ep: 8 (over z, y), tp: 4 (over x, core).
Axes of the slice: x: 2, y: 2, z: 4, core: 2. Of those that a mesh axis runs over, the one named last changes fastest.
Arguments:
- queries: bfloat16 [8192, 1024], P('ep', 'tp'), may hold values from -6 to 6
- key_rows: bfloat16 [8192, 256], P('ep', 'tp'), may hold values from -6 to 6
- values: bfloat16 [8192, 256], P('ep', 'tp'), may hold values from -6 to 6
- sink_logit: float32 [16], P('tp'), may hold values from 3 to 7
- out_weight: bfloat16 [1024, 2048], P('tp'), may hold values from -0.1875 to 0.1875
- out_gain: float32 [2048], replicated, may hold values from 0.1 to 1.9
- routed_tokens: bfloat16 [16384, 2048], P(('ep', 'tp')), may hold values from -6 to 6
- expert_ids: int32 [16384, 2], P(('ep', 'tp')), may hold values from 0 to 31, as said below
- route_weight: float32 [16384, 2], P(('ep', 'tp')), may hold values from 0.1 to 1
- routed_gain: float32 [2048], replicated, may hold values from 0.1 to 1.9
- expert_gate: bfloat16 [32, 2048, 1024], P('ep', None, 'tp'), may hold values from -0.125 to 0.125
- expert_up: bfloat16 [32, 2048, 1024], P('ep', None, 'tp'), may hold values from -0.125 to 0.125
- expert_down: bfloat16 [32, 2048, 1024], P('ep', None, 'tp'), may hold values from -0.1875 to 0.1875
Outputs:
- mixer_out: bfloat16 [8192, 2048], P(('ep', 'tp'))
- experts_out: bfloat16 [16384, 2048], P(('ep', 'tp'))
The draws below stay inside these ranges and needn't reach their ends.
Inputs may be any that keep to these rules, and one draw needn't show every extreme that they name: `expert_ids`: both experts of a row lie in one group (equal id // 8); the 512 rows of one device name every group exactly 512 / 4 times; the rows of one device name no expert more than 64 times; in every device's rows some expert of each group is named exactly 64 times, and one expert is named exactly 64 times by the rows of every device.
All inputs are finite; a program needn't handle non-finite values.
Results may differ from the reference program's by a relative error of at most 0.0071.
Values may be sent and summed in bfloat16 or wider, within the bound.
A program may use at most 192 MiB of HBM per device.

```python
import math
import jax
import jax.numpy as jnp
from jax import lax

D = 2048
HEADS = 16
KV_HEADS = 4
HEAD_DIM = 64
WINDOW = 128
QBLOCK = 512
EXPERTS = 32
GROUPS = 4
EPG = 8
TOP = 2
EXPERT_FF = 1024
TB = 512
CAP = 64
SEQ_A = 8192
TOKENS_B = 16384
N_EP = 8
N_TP = 4


def draw_queries(key, part):
    drawn = jax.random.normal(jax.random.fold_in(key, 12), (SEQ_A, HEADS * HEAD_DIM), jnp.float32)
    return jnp.clip(drawn, -4.0, 4.0).astype(jnp.bfloat16)


def draw_key_rows(key, part):
    drawn = jax.random.normal(jax.random.fold_in(key, 22), (SEQ_A, KV_HEADS * HEAD_DIM), jnp.float32)
    return jnp.clip(drawn, -4.0, 4.0).astype(jnp.bfloat16)


def draw_expert_ids(key, part):
    block_total = TOKENS_B // TB
    half_group = TB // (2 * GROUPS)
    common_hot = jax.random.randint(jax.random.fold_in(key, 101), (), 0, EPG)

    def one_block(block_index):
        block_key = jax.random.fold_in(jax.random.fold_in(key, 202), block_index)
        order_key, hot_key, rest_key = jax.random.split(block_key, 3)
        order = jax.random.permutation(order_key, TB)
        hottest = jax.random.randint(hot_key, (GROUPS,), 0, EPG).at[0].set(common_hot)
        others = jax.vmap(lambda inner: jax.random.permutation(inner, EPG - 1))(jax.random.split(rest_key, GROUPS))
        group = order % GROUPS
        rank = order // GROUPS
        hot_token = hottest[group]
        rest_token = others[group]
        stride = 1 + rank // (EPG - 1) % (EPG - 2)
        first_other = jnp.take_along_axis(rest_token, (rank % (EPG - 1))[:, None], axis=1)[:, 0]
        second_other = jnp.take_along_axis(rest_token, ((rank + stride) % (EPG - 1))[:, None], axis=1)[:, 0]
        other_one = (hot_token + 1 + first_other) % EPG
        other_two = (hot_token + 1 + second_other) % EPG
        leading = jnp.where(rank < half_group, hot_token, other_one)
        trailing = jnp.where(rank < half_group, other_one, other_two)
        return jnp.stack([group * EPG + leading, group * EPG + trailing], axis=-1)
    chosen = jax.vmap(one_block)(jnp.arange(block_total))
    return chosen.reshape(TOKENS_B, TOP).astype(jnp.int32)


def block_scale(rng, dims, shards, least, high):
    gain = 1.0
    for dim, blocks in shards:
        steps = jax.random.uniform(jax.random.fold_in(jax.random.fold_in(rng, 6), dim), (blocks,), jnp.float32, least / len(shards), high / len(shards))
        gain = gain * jnp.repeat(jnp.exp(steps), dims[dim] // blocks).reshape((-1,) + (1,) * (len(dims) - 1 - dim))
    return gain


def gaussian(rng, shape, deviation, most, cuts=(), kind=jnp.bfloat16):
    level = block_scale(rng, shape, cuts, -0.22, 0.18) if cuts else 1.0
    values = jax.random.normal(rng, shape, jnp.float32) * deviation * level
    return jnp.minimum(jnp.maximum(values, -most), most).astype(kind)


def setup_inputs(seed: int = 0) -> dict:
    seeds = jax.random.split(jax.random.key(seed), 14)
    queries = draw_queries(jax.random.fold_in(seeds[13], 71), 0)
    key_rows = draw_key_rows(jax.random.fold_in(seeds[13], 71), 0)
    values = gaussian(seeds[2], (SEQ_A, KV_HEADS * HEAD_DIM), 1.0, 6.0, ((0, 8), (1, 4)))
    sink_logit = jnp.clip(3.0 + 4.0 * jax.random.uniform(seeds[3], (HEADS,), jnp.float32) ** block_scale(seeds[3], (HEADS,), ((0, 4),), -0.2, 0.2), 3.0, 7.0)
    out_weight = gaussian(seeds[4], (HEADS * HEAD_DIM, D), (HEADS * HEAD_DIM) ** -0.5, 0.1875, ((0, 4),))
    out_gain = jnp.clip(1.0 + 0.18 * jax.random.normal(seeds[5], (D,), jnp.float32), 0.1, 1.9)
    routed_tokens = gaussian(seeds[6], (TOKENS_B, D), 1.0, 6.0, ((0, 32),))
    expert_ids = draw_expert_ids(jax.random.fold_in(seeds[13], 71), 0)
    route_weight = jnp.clip(jnp.exp(math.log(1.0) - 2.3025851 * jax.random.uniform(seeds[8], (TOKENS_B, TOP), jnp.float32) ** block_scale(seeds[8], (TOKENS_B, TOP), ((0, 32),), -0.2, 0.2)), 0.1, 1.0)
    routed_gain = jnp.clip(1.0 + 0.18 * jax.random.normal(seeds[9], (D,), jnp.float32), 0.1, 1.9)
    expert_gate = gaussian(seeds[10], (EXPERTS, D, EXPERT_FF), D ** -0.5, 0.125, ((0, 8), (2, 4)))
    expert_up = gaussian(seeds[11], (EXPERTS, D, EXPERT_FF), D ** -0.5, 0.125, ((0, 8), (2, 4)))
    expert_down = gaussian(seeds[12], (EXPERTS, D, EXPERT_FF), EXPERT_FF ** -0.5, 0.1875, ((0, 8), (2, 4)))
    return dict(queries=queries, key_rows=key_rows, values=values, sink_logit=sink_logit, out_weight=out_weight, out_gain=out_gain, routed_tokens=routed_tokens, expert_ids=expert_ids, route_weight=route_weight, routed_gain=routed_gain, expert_gate=expert_gate, expert_up=expert_up, expert_down=expert_down)


epsilon = 1e-06
far_below = -1e+30

def window_block(block_index, grouped, padded_keys, padded_values, sink_logit, seq_total):
    start_row = block_index * QBLOCK
    span_keys = QBLOCK + 2 * WINDOW
    query_block = lax.dynamic_slice_in_dim(grouped, start_row, QBLOCK, 0).astype(jnp.float32)
    key_block = lax.dynamic_slice_in_dim(padded_keys, start_row, span_keys, 0).astype(jnp.float32)
    value_block = lax.dynamic_slice_in_dim(padded_values, start_row, span_keys, 0).astype(jnp.float32)
    scores = jnp.einsum('qhgd,khd->hgqk', query_block, key_block) * HEAD_DIM ** (-0.5)
    query_pos = start_row + jnp.arange(QBLOCK, dtype=jnp.int32)
    key_pos = start_row - WINDOW + jnp.arange(span_keys, dtype=jnp.int32)
    valid = (jnp.abs(key_pos[None, :] - query_pos[:, None]) <= WINDOW) & (key_pos[None, :] >= 0) & (key_pos[None, :] < seq_total)
    sinks = sink_logit.reshape(KV_HEADS, HEADS // KV_HEADS)[:, :, None, None]
    masked = jnp.where(valid, scores, far_below)
    largest = jnp.maximum(lax.optimization_barrier(jnp.max(masked, axis=-1, keepdims=True)), sinks)
    raised = jnp.where(valid, jnp.exp(masked - largest), 0.0)
    denominator = lax.optimization_barrier(jnp.sum(raised, axis=-1, keepdims=True)) + jnp.exp(sinks - largest)
    weights = (raised / denominator).astype(jnp.bfloat16)
    attended = jnp.einsum('hgqk,khd->qhgd', weights.astype(jnp.float32), value_block)
    return attended.astype(jnp.bfloat16).reshape(QBLOCK, HEADS * HEAD_DIM)

def reference(queries, key_rows, values, sink_logit, out_weight, out_gain, routed_tokens, expert_ids, route_weight, routed_gain, expert_gate, expert_up, expert_down):
    seq_total = queries.shape[0]
    grouped = queries.reshape(seq_total, KV_HEADS, HEADS // KV_HEADS, HEAD_DIM)
    padding = ((WINDOW, WINDOW), (0, 0), (0, 0))
    padded_keys = jnp.pad(key_rows.reshape(seq_total, KV_HEADS, HEAD_DIM), padding)
    padded_values = jnp.pad(values.reshape(seq_total, KV_HEADS, HEAD_DIM), padding)
    block_ids = jnp.arange(seq_total // QBLOCK, dtype=jnp.int32)
    attended = lax.map(lambda block_index: window_block(block_index, grouped, padded_keys, padded_values, sink_logit, seq_total), block_ids)
    attended = attended.reshape(seq_total, HEADS * HEAD_DIM)
    mixed = jnp.dot(attended, out_weight, preferred_element_type=jnp.float32)
    mixer_out = (mixed * lax.rsqrt(lax.optimization_barrier(jnp.mean(mixed * mixed, axis=-1, keepdims=True)) + epsilon) * out_gain).astype(jnp.bfloat16)
    token_total = routed_tokens.shape[0]
    inputs = routed_tokens.astype(jnp.float32)
    normed = (inputs * lax.rsqrt(lax.optimization_barrier(jnp.mean(inputs * inputs, axis=-1, keepdims=True)) + epsilon) * routed_gain).astype(jnp.bfloat16)
    flat_ids = expert_ids.reshape(-1)
    most_rows = CAP * N_EP * N_TP
    empty = jnp.zeros((token_total * TOP, normed.shape[1]), jnp.bfloat16)

    def one_expert(results, expert):
        picked = jnp.nonzero(flat_ids == expert, size=most_rows, fill_value=token_total * TOP)[0]
        rows_in = jnp.take(normed, picked // TOP, axis=0, mode='fill', fill_value=0)
        gate = jnp.dot(rows_in, expert_gate[expert], preferred_element_type=jnp.float32)
        upward = jnp.dot(rows_in, expert_up[expert], preferred_element_type=jnp.float32)
        hidden = (jax.nn.silu(gate) * upward).astype(jnp.bfloat16)
        produced = jnp.dot(hidden, expert_down[expert].T, preferred_element_type=jnp.float32).astype(jnp.bfloat16)
        return (results.at[picked].set(produced, mode='drop'), None)
    results, unused = lax.scan(one_expert, empty, jnp.arange(EXPERTS, dtype=jnp.int32))
    results = results.reshape(token_total, TOP, normed.shape[1]).astype(jnp.float32)
    experts_out = lax.optimization_barrier(jnp.sum(results * route_weight[:, :, None], axis=1)).astype(jnp.bfloat16)
    return (mixer_out, experts_out)
```

```python
import functools

import jax
import jax.numpy as jnp
from jax import lax
from jax.experimental import pallas as pl
from jax.experimental.pallas import tpu as pltpu
from jax.sharding import Mesh, PartitionSpec as P

HEAD_DIM = 64
WINDOW = 128
QBLOCK = 512
EXPERTS = 32
EPG = 8
TOP = 2
GROUPS = EXPERTS // EPG
CHUNK_ROWS = 2048
ROW_TILE = 512

epsilon = 1e-06
EP = ("group", "member")
PLANE = ("member", "tp")


def padded(block, width):
    count = lax.axis_size(EP)
    forward = [(i, i + 1) for i in range(count - 1)]
    backward = [(target, source) for source, target in forward]
    low = lax.ppermute(block[-width:], EP, forward)
    high = lax.ppermute(block[:width], EP, backward)
    return jnp.concatenate([low, block, high], axis=0)


def attention(queries, key_rows, values, sink_logit):
    row_count = queries.shape[0]
    heads_here = queries.shape[1] // HEAD_DIM
    kv_here = key_rows.shape[1] // HEAD_DIM
    group_size = heads_here // kv_here
    paired = jnp.concatenate((key_rows, values), axis=1)
    extended = padded(paired, WINDOW)
    offset = lax.axis_index(EP) * row_count
    seq_total = row_count * lax.axis_size(EP)
    grouped = queries.reshape(row_count, kv_here, group_size, HEAD_DIM)
    sinks = sink_logit.reshape(kv_here, group_size)[:, :, None, None]
    span_keys = QBLOCK + 2 * WINDOW

    def attend_block(block_index):
        start_row = block_index * QBLOCK
        query_block = lax.dynamic_slice_in_dim(grouped, start_row, QBLOCK, 0)
        band = lax.dynamic_slice_in_dim(extended, start_row, span_keys, 0)
        key_block = band[:, : kv_here * HEAD_DIM].reshape(span_keys, kv_here, HEAD_DIM)
        value_block = band[:, kv_here * HEAD_DIM :].reshape(span_keys, kv_here, HEAD_DIM)
        scores = jnp.einsum(
            "qhgd,khd->hgqk", query_block, key_block, preferred_element_type=jnp.float32
        ) * HEAD_DIM ** (-0.5)
        query_pos = offset + start_row + jnp.arange(QBLOCK, dtype=jnp.int32)
        key_pos = offset + start_row - WINDOW + jnp.arange(span_keys, dtype=jnp.int32)
        valid = (
            (jnp.abs(key_pos[None, :] - query_pos[:, None]) <= WINDOW)
            & (key_pos[None, :] >= 0)
            & (key_pos[None, :] < seq_total)
        )
        masked = jnp.where(valid, scores, -1e30)
        largest = jnp.maximum(jnp.max(masked, axis=-1, keepdims=True), sinks)
        raised = jnp.where(valid, jnp.exp(masked - largest), 0.0)
        denominator = jnp.sum(raised, axis=-1, keepdims=True) + jnp.exp(sinks - largest)
        weights = (raised / denominator).astype(jnp.bfloat16)
        attended = jnp.einsum(
            "hgqk,khd->qhgd", weights, value_block, preferred_element_type=jnp.float32
        )
        return attended.astype(jnp.bfloat16).reshape(QBLOCK, heads_here * HEAD_DIM)

    attended = lax.map(attend_block, jnp.arange(row_count // QBLOCK, dtype=jnp.int32))
    attended = attended.reshape(row_count, heads_here * HEAD_DIM)
    return lax.all_to_all(attended, "tp", split_axis=0, concat_axis=1, tiled=True)


def project(attended, full_weight, out_gain):
    mixed = jnp.dot(attended, full_weight, preferred_element_type=jnp.float32)
    return (
        mixed * lax.rsqrt(jnp.mean(mixed * mixed, axis=-1, keepdims=True) + epsilon) * out_gain
    ).astype(jnp.bfloat16)


def expert_kernel(x_ref, w_ref, gate_ref, up_ref, down_ref, out_ref, total):
    x = x_ref[...]
    for e in range(gate_ref.shape[0]):
        gate = jnp.dot(x, gate_ref[e], preferred_element_type=jnp.float32)
        upward = jnp.dot(x, up_ref[e], preferred_element_type=jnp.float32)
        hidden = (gate / (1.0 + jnp.exp(-gate)) * upward * w_ref[:, e : e + 1]).astype(
            jnp.bfloat16
        )
        part = lax.dot_general(
            hidden, down_ref[e], (((1,), (1,)), ((), ())), preferred_element_type=jnp.float32
        )
        if e == 0:
            total[...] = part
        else:
            total[...] += part
    out_ref[...] = total[...].astype(jnp.bfloat16)


def apply_experts(rows, weights, gate, up, down):
    count, width = rows.shape
    local_experts, _, units = gate.shape
    tile = min(ROW_TILE, count)
    whole = lambda i: (0, 0, 0)
    return pl.pallas_call(
        expert_kernel,
        grid=(count // tile,),
        out_shape=jax.ShapeDtypeStruct((count, width), jnp.bfloat16),
        in_specs=[
            pl.BlockSpec((tile, width), lambda i: (i, 0)),
            pl.BlockSpec((tile, local_experts), lambda i: (i, 0)),
            pl.BlockSpec(gate.shape, whole, pipeline_mode=pl.Buffered(1)),
            pl.BlockSpec(up.shape, whole, pipeline_mode=pl.Buffered(1)),
            pl.BlockSpec(down.shape, whole, pipeline_mode=pl.Buffered(1)),
        ],
        out_specs=pl.BlockSpec((tile, width), lambda i: (i, 0)),
        scratch_shapes=[pltpu.VMEM((tile, width), jnp.float32)],
        compiler_params=pltpu.CompilerParams(vmem_limit_bytes=48 * 2**20),
        cost_estimate=pl.CostEstimate(
            flops=6 * count * width * local_experts * units,
            bytes_accessed=4 * count * width + 6 * local_experts * units * width,
            transcendentals=count * local_experts * units,
        ),
    )(rows, weights, gate, up, down)


def routed(tokens, expert_ids, route_weight, gain, gate, up, down, full_weight, attended):
    token_total, width = tokens.shape
    share = token_total // GROUPS
    plane = lax.axis_size(PLANE)
    local_experts = gate.shape[0]
    inputs = tokens.astype(jnp.float32)
    normed = (
        inputs * lax.rsqrt(jnp.mean(inputs * inputs, axis=-1, keepdims=True) + epsilon) * gain
    ).astype(jnp.bfloat16)
    group = expert_ids[:, 0] // EPG
    in_group = (group[:, None] == jnp.arange(GROUPS, dtype=jnp.int32)).astype(jnp.float32)
    index = jnp.arange(token_total, dtype=jnp.int32)
    before = (index[None, :] < index[:, None]).astype(jnp.float32)
    ranks = jnp.dot(before, in_group, preferred_element_type=jnp.float32)
    rank = jnp.sum(ranks * in_group, axis=1).astype(jnp.int32)
    position = group * share + rank
    order = (position[None, :] == index[:, None]).astype(jnp.bfloat16)
    back = (position[:, None] == index[None, :]).astype(jnp.bfloat16)
    ordered = jnp.dot(order, normed, preferred_element_type=jnp.float32).astype(jnp.bfloat16)
    member = jnp.arange(EPG, dtype=jnp.int32)
    spread = jnp.sum(
        jnp.where((expert_ids % EPG)[:, :, None] == member, route_weight[:, :, None], 0.0), axis=1
    )
    spread = jnp.dot(
        order.astype(jnp.float32), spread, precision=lax.Precision.HIGHEST,
        preferred_element_type=jnp.float32,
    )
    spread = spread.reshape(GROUPS, share, EPG).transpose(0, 2, 1).reshape(GROUPS, EPG * share)
    spread = lax.all_to_all(spread, "group", 0, 0, tiled=True)
    spread = lax.all_gather(spread, PLANE, axis=0, tiled=True)
    spread = spread.reshape(plane, GROUPS, EPG, share)
    mine = lax.dynamic_slice_in_dim(
        spread, lax.axis_index("member") * local_experts, local_experts, 2
    ).transpose(0, 1, 3, 2)
    piece = max(min(share, CHUNK_ROWS // (plane * GROUPS)), 16)
    ordered = ordered.reshape(GROUPS, share, width)
    mine, attended = lax.optimization_barrier((mine, attended))
    results = []
    for start in range(0, share, piece):
        sent = lax.all_to_all(ordered[:, start : start + piece], "group", 0, 0, tiled=True)
        sent = sent.reshape(GROUPS * piece, width)
        if start == 0:
            sent, full_weight = lax.optimization_barrier((sent, full_weight))
        rows = lax.all_gather(sent, PLANE, axis=0, tiled=True)
        weights = mine[:, :, start : start + piece].reshape(plane * GROUPS * piece, local_experts)
        partial = apply_experts(rows, weights, gate, up, down)
        summed = lax.psum_scatter(partial, PLANE, scatter_dimension=0, tiled=True)
        summed = summed.reshape(GROUPS, piece, width)
        results.append(lax.all_to_all(summed, "group", 0, 0, tiled=True))
    result = jnp.concatenate(results, axis=1).reshape(token_total, width)
    result = jnp.dot(back, result, preferred_element_type=jnp.float32).astype(jnp.bfloat16)
    return result, full_weight, attended


MESH = pl.DeviceIdType.MESH
QUAD = 4
PART_ROWS = 64


def fused_experts(steps, rows, ordered, spread, gate, up, down, out,
                  xbuf, wraw, wcol, wg, wu, wd, hid, own, part, got1, got2, fin,
                  send, recv, wsem, ssem):
    plane, member, place = (lax.axis_index(a) for a in ("group", "member", "tp"))
    experts, width, units = gate.shape
    share = spread.shape[-1]
    here = experts * units
    blocks = 2 * experts
    first = rows // 2

    def device(dz=0, dx=0, dy=0, dcore=0):
        z = (plane // 2 + dz // 2) % 2 * 2 + (plane % 2 + dz % 2) % 2
        t = (place // 2 + dx) % 2 * 2 + (place % 2 + dcore) % 2
        return (z, (member + dy) % 2, t)

    def far(s):
        return (s + s // GROUPS) % GROUPS

    def slot(q, start=0, count=rows):
        return pl.ds(pl.multiple_of(q * rows + start, 16), count)

    def remote(src, dst, s, k, target):
        return pltpu.make_async_remote_copy(
            src_ref=src, dst_ref=dst, send_sem=send.at[s, k], recv_sem=recv.at[s, k],
            device_id=target, device_id_type=MESH,
        )

    def tokens_of(s):
        return pl.ds(pl.multiple_of(far(s) * share + s // GROUPS * rows, 16), rows)

    def local_in(s):
        return pltpu.make_async_copy(
            ordered.at[tokens_of(s)], xbuf.at[s, slot(0)], recv.at[s, 0]
        )

    def dispatch(s):
        return remote(ordered.at[tokens_of(s)], xbuf.at[s, slot(0)], s, 0, device(far(s)))

    def to_x(s):
        return remote(xbuf.at[s, slot(0)], xbuf.at[s, slot(1)], s, 1, device(dx=1))

    def to_y(s):
        return remote(xbuf.at[s, slot(0)], xbuf.at[s, slot(2)], s, 2, device(dy=1))

    def pass_y(s):
        return remote(
            xbuf.at[s, slot(1, 0, first)], xbuf.at[s, slot(3, 0, first)], s, 3, device(dy=1)
        )

    def pass_x(s):
        return remote(
            xbuf.at[s, slot(2, first, rows - first)],
            xbuf.at[s, slot(3, first, rows - first)], s, 4, device(dx=1),
        )

    def corner_x(s):
        return remote(
            part.at[s, slot(2, 0, first)], got1.at[s, pl.ds(0, first)], s, 5, device(dx=1)
        )

    def corner_y(s):
        return remote(
            part.at[s, slot(2, first, rows - first)], got1.at[s, pl.ds(first, rows - first)],
            s, 6, device(dy=1),
        )

    def sum_x(s):
        return remote(part.at[s, slot(0)], got2.at[s, slot(0)], s, 7, device(dx=1))

    def sum_y(s):
        return remote(part.at[s, slot(1)], got2.at[s, slot(1)], s, 8, device(dy=1))

    def give_back(s):
        return remote(fin.at[s], out.at[tokens_of(s)], s, 9, device(far(s)))

    def local_out(s):
        return pltpu.make_async_copy(fin.at[s], out.at[tokens_of(s)], recv.at[s, 9])

    def weight_refs(e, to):
        at = to * experts + e
        return (
            (gate.at[e], wg.at[at]),
            (up.at[e], wu.at[at]),
            (down.at[e], wd.at[:, pl.ds(at * units, units)]),
        )

    def weight_copies():
        for e in range(experts):
            for n, (src, dst) in enumerate(weight_refs(e, 0)):
                yield pltpu.make_async_copy(src, dst, wsem.at[0, 3 * e + n])
            for n, (src, dst) in enumerate(weight_refs(e, 1)):
                yield pltpu.make_async_remote_copy(
                    src_ref=src, dst_ref=dst, send_sem=wsem.at[1, 3 * e + n],
                    recv_sem=wsem.at[2, 3 * e + n], device_id=device(dcore=1),
                    device_id_type=MESH,
                )

    def spread_copies():
        for dz in range(GROUPS):
            for q in range(QUAD):
                dx, dy = q % 2, q // 2
                src, dst, n = spread.at[dy, dz], wraw.at[dz, q], dz * QUAD + q
                if n == 0:
                    yield pltpu.make_async_copy(src, dst, ssem.at[1, n])
                else:
                    yield pltpu.make_async_remote_copy(
                        src_ref=src, dst_ref=dst, send_sem=ssem.at[0, n], recv_sem=ssem.at[1, n],
                        device_id=device(dz, dx, dy), device_id_type=MESH,
                    )

    barrier = pltpu.get_barrier_semaphore()
    peers = [(z, q % 2, q // 2, 0) for z in range(GROUPS) for q in range(QUAD)][1:] + [(0, 0, 0, 1)]
    for peer in peers:
        pl.semaphore_signal(barrier, inc=1, device_id=device(*peer), device_id_type=MESH)
    pl.semaphore_wait(barrier, len(peers))

    for s in range(steps):
        if far(s) == 0:
            local_in(s).start()
    for s in range(steps):
        if far(s) != 0:
            dispatch(s).start()
    for copy in spread_copies():
        copy.start()
    for copy in weight_copies():
        copy.start()

    def gather(s):
        @pl.when(far(s) == 0)
        def _():
            local_in(s).wait()

        @pl.when(far(s) != 0)
        def _():
            dispatch(s).wait_recv()

        to_x(s).start()
        to_y(s).start()

    def forward(s):
        to_x(s).wait_recv()
        pass_y(s).start()
        to_y(s).wait_recv()
        pass_x(s).start()

    gather(0)
    gather(1)
    forward(0)

    for copy in spread_copies():
        if hasattr(copy, "wait_recv") and copy.is_remote:
            copy.wait_recv()
        else:
            copy.wait()
    for dz in range(GROUPS):
        for q in range(QUAD):
            turned = wraw[dz, q].T
            for piece in range(share // rows):
                s = piece * GROUPS + (dz - piece) % GROUPS
                wcol[s, q * rows : (q + 1) * rows, :] = turned[piece * rows : (piece + 1) * rows]
    for copy in weight_copies():
        if copy.is_remote:
            copy.wait_recv()
        else:
            copy.wait()

    def compute(s):
        for j in range(blocks):
            x = xbuf[s]
            g = jnp.dot(x, wg[j], preferred_element_type=jnp.float32)
            u = jnp.dot(x, wu[j], preferred_element_type=jnp.float32)
            e = j % experts
            h = g / (1.0 + jnp.exp(-g)) * u * wcol[s, :, e : e + 1]
            hid[:, j * units : (j + 1) * units] = h.astype(jnp.bfloat16)
        step = 256

        @pl.loop(0, width // step)
        def _(n):
            columns = pl.ds(pl.multiple_of(n * step, step), step)
            p = lax.dot_general(
                hid[...], wd[columns, :], (((1,), (1,)), ((), ())),
                preferred_element_type=jnp.float32,
            )
            own[s % 3, :, columns] = p[:rows]
            part[s, :, columns] = p[rows:].astype(jnp.bfloat16)

    def settle(s):
        corner_x(s).wait_recv()
        held = part[s, rows : rows + first].astype(jnp.float32)
        part[s, rows : rows + first] = (
            held + got1[s, :first].astype(jnp.float32)
        ).astype(jnp.bfloat16)
        sum_y(s).start()
        corner_y(s).wait_recv()
        held = part[s, first:rows].astype(jnp.float32)
        part[s, first:rows] = (held + got1[s, first:].astype(jnp.float32)).astype(jnp.bfloat16)
        sum_x(s).start()

    def finish(s):
        sum_y(s).wait_recv()
        sum_x(s).wait_recv()
        fin[s] = (
            own[s % 3] + got2[s, :rows].astype(jnp.float32) + got2[s, rows:].astype(jnp.float32)
        ).astype(jnp.bfloat16)

        @pl.when(far(s) == 0)
        def _():
            local_out(s).start()

        @pl.when(far(s) != 0)
        def _():
            give_back(s).start()

    @pl.loop(0, steps + 2)
    def _(i):
        @pl.when(i + 2 < steps)
        def _():
            gather(i + 2)

        @pl.when(i + 1 < steps)
        def _():
            forward(i + 1)

        @pl.when(i >= 2)
        def _():
            finish(i - 2)

        @pl.when(i < steps)
        def _():
            pass_y(i).wait_recv()
            pass_x(i).wait_recv()
            compute(i)
            corner_x(i).start()
            corner_y(i).start()

        @pl.when(jnp.logical_and(i >= 1, i < steps + 1))
        def _():
            settle(i - 1)

    for copy in spread_copies():
        if copy.is_remote:
            copy.wait_send()
    for copy in weight_copies():
        if copy.is_remote:
            copy.wait_send()

    @pl.loop(0, steps)
    def _(s):
        for copy in (to_x, to_y, pass_y, pass_x, corner_x, corner_y, sum_x, sum_y):
            copy(s).wait_send()

        @pl.when(far(s) == 0)
        def _():
            local_out(s).wait()

        @pl.when(far(s) != 0)
        def _():
            dispatch(s).wait_send()
            give_back(s).wait()


def apply_fused(ordered, spread, gate, up, down):
    total, width = ordered.shape
    experts, _, units = gate.shape
    share = total // GROUPS
    rows = min(PART_ROWS, share)
    steps = total // rows
    hidden = 2 * experts * units
    anywhere = pl.BlockSpec(memory_space=pl.ANY)
    dma = pltpu.SemaphoreType.DMA
    return pl.pallas_call(
        functools.partial(fused_experts, steps, rows),
        out_shape=jax.ShapeDtypeStruct((total, width), jnp.bfloat16),
        in_specs=[anywhere] * 5,
        out_specs=anywhere,
        scratch_shapes=[
            pltpu.VMEM((steps, QUAD * rows, width), jnp.bfloat16),
            pltpu.VMEM((GROUPS, QUAD) + spread.shape[-2:], jnp.float32),
            pltpu.VMEM((steps, QUAD * rows, EPG), jnp.float32),
            pltpu.VMEM((2 * experts, width, units), jnp.bfloat16),
            pltpu.VMEM((2 * experts, width, units), jnp.bfloat16),
            pltpu.VMEM((width, hidden), jnp.bfloat16),
            pltpu.VMEM((QUAD * rows, hidden), jnp.bfloat16),
            pltpu.VMEM((3, rows, width), jnp.float32),
            pltpu.VMEM((steps, (QUAD - 1) * rows, width), jnp.bfloat16),
            pltpu.VMEM((steps, rows, width), jnp.bfloat16),
            pltpu.VMEM((steps, 2 * rows, width), jnp.bfloat16),
            pltpu.VMEM((steps, rows, width), jnp.bfloat16),
            dma((steps, 10)),
            dma((steps, 10)),
            dma((3, 3 * experts)),
            dma((2, GROUPS * QUAD)),
        ],
        compiler_params=pltpu.CompilerParams(
            collective_id=0, has_side_effects=True, vmem_limit_bytes=66 * 10**6
        ),
        cost_estimate=pl.CostEstimate(
            flops=6 * QUAD * total * width * hidden,
            bytes_accessed=6 * experts * units * width,
            transcendentals=QUAD * total * hidden,
        ),
    )(ordered, spread, gate, up, down)


def routed_fused(tokens, expert_ids, route_weight, gain, gate, up, down):
    token_total, width = tokens.shape
    share = token_total // GROUPS
    local_experts = gate.shape[0]
    inputs = tokens.astype(jnp.float32)
    normed = (
        inputs * lax.rsqrt(jnp.mean(inputs * inputs, axis=-1, keepdims=True) + epsilon) * gain
    ).astype(jnp.bfloat16)
    group = jnp.bitwise_xor(expert_ids[:, 0] // EPG, lax.axis_index("group"))
    in_group = (group[:, None] == jnp.arange(GROUPS, dtype=jnp.int32)).astype(jnp.float32)
    index = jnp.arange(token_total, dtype=jnp.int32)
    before = (index[None, :] < index[:, None]).astype(jnp.float32)
    ranks = jnp.dot(before, in_group, preferred_element_type=jnp.float32)
    rank = jnp.sum(ranks * in_group, axis=1).astype(jnp.int32)
    position = group * share + rank
    order = (position[None, :] == index[:, None]).astype(jnp.bfloat16)
    back = (position[:, None] == index[None, :]).astype(jnp.bfloat16)
    ordered = jnp.dot(order, normed, preferred_element_type=jnp.float32).astype(jnp.bfloat16)
    start = lax.axis_index("member") * local_experts
    member = (jnp.arange(EPG, dtype=jnp.int32) + start) % EPG
    spread = jnp.sum(
        jnp.where((expert_ids % EPG)[:, :, None] == member, route_weight[:, :, None], 0.0), axis=1
    )
    spread = jnp.dot(
        order.astype(jnp.float32), spread, precision=lax.Precision.HIGHEST,
        preferred_element_type=jnp.float32,
    )
    spread = spread.reshape(GROUPS, share, EPG).transpose(0, 2, 1)
    spread = jnp.stack([spread, jnp.roll(spread, local_experts, axis=1)])
    result = apply_fused(ordered, spread, gate, up, down)
    return jnp.dot(back, result, preferred_element_type=jnp.float32).astype(jnp.bfloat16)


def local(queries, key_rows, values, sink_logit, out_weight, out_gain, routed_tokens,
          expert_ids, route_weight, routed_gain, expert_gate, expert_up, expert_down):
    full_weight = lax.all_gather(out_weight, "tp", axis=0, tiled=True)
    attended = attention(queries, key_rows, values, sink_logit)
    if lax.axis_size("member") == 2 and lax.axis_size("tp") == 4:
        experts_out = routed_fused(
            routed_tokens, expert_ids, route_weight, routed_gain, expert_gate, expert_up,
            expert_down,
        )
        return (project(attended, full_weight, out_gain), experts_out)
    experts_out, full_weight, attended = routed(
        routed_tokens, expert_ids, route_weight, routed_gain, expert_gate, expert_up, expert_down,
        full_weight, attended,
    )
    mixer_out = project(attended, full_weight, out_gain)
    return (mixer_out, experts_out)


def solution(mesh):
    ep, tp = mesh.shape["ep"], mesh.shape["tp"]
    split = Mesh(mesh.devices.reshape(GROUPS, ep // GROUPS, tp), ("group", "member", "tp"))
    every = ("group", "member", "tp")
    placed = (
        P(EP, "tp"),
        P(EP, "tp"),
        P(EP, "tp"),
        P("tp"),
        P("tp", None),
        P(),
        P(every, None),
        P(every, None),
        P(every, None),
        P(),
        P(EP, None, "tp"),
        P(EP, None, "tp"),
        P(EP, None, "tp"),
    )
    return jax.shard_map(
        local,
        mesh=split,
        in_specs=placed,
        out_specs=(P(every, None), P(every, None)),
        check_vma=False,
    )
```

```python
import functools

import jax
import jax.numpy as jnp
from jax import lax
from jax.experimental import pallas as pl
from jax.experimental.pallas import tpu as pltpu
from jax.sharding import Mesh, PartitionSpec as P

HEAD_DIM = 64
WINDOW = 128
QBLOCK = 512
EXPERTS = 32
EPG = 8
TOP = 2
GROUPS = EXPERTS // EPG
CHUNK_ROWS = 2048
ROW_TILE = 512

epsilon = 1e-06
EP = ("group", "member")
PLANE = ("member", "tp")


def padded(block, width):
    count = lax.axis_size(EP)
    forward = [(i, i + 1) for i in range(count - 1)]
    backward = [(target, source) for source, target in forward]
    low = lax.ppermute(block[-width:], EP, forward)
    high = lax.ppermute(block[:width], EP, backward)
    return jnp.concatenate([low, block, high], axis=0)


def attention(queries, key_rows, values, sink_logit):
    row_count = queries.shape[0]
    heads_here = queries.shape[1] // HEAD_DIM
    kv_here = key_rows.shape[1] // HEAD_DIM
    group_size = heads_here // kv_here
    paired = jnp.concatenate((key_rows, values), axis=1)
    extended = padded(paired, WINDOW)
    offset = lax.axis_index(EP) * row_count
    seq_total = row_count * lax.axis_size(EP)
    grouped = queries.reshape(row_count, kv_here, group_size, HEAD_DIM)
    sinks = sink_logit.reshape(kv_here, group_size)[:, :, None, None]
    span_keys = QBLOCK + 2 * WINDOW

    def attend_block(block_index):
        start_row = block_index * QBLOCK
        query_block = lax.dynamic_slice_in_dim(grouped, start_row, QBLOCK, 0)
        band = lax.dynamic_slice_in_dim(extended, start_row, span_keys, 0)
        key_block = band[:, : kv_here * HEAD_DIM].reshape(span_keys, kv_here, HEAD_DIM)
        value_block = band[:, kv_here * HEAD_DIM :].reshape(span_keys, kv_here, HEAD_DIM)
        scores = jnp.einsum(
            "qhgd,khd->hgqk", query_block, key_block, preferred_element_type=jnp.float32
        ) * HEAD_DIM ** (-0.5)
        query_pos = offset + start_row + jnp.arange(QBLOCK, dtype=jnp.int32)
        key_pos = offset + start_row - WINDOW + jnp.arange(span_keys, dtype=jnp.int32)
        valid = (
            (jnp.abs(key_pos[None, :] - query_pos[:, None]) <= WINDOW)
            & (key_pos[None, :] >= 0)
            & (key_pos[None, :] < seq_total)
        )
        masked = jnp.where(valid, scores, -1e30)
        largest = jnp.maximum(jnp.max(masked, axis=-1, keepdims=True), sinks)
        raised = jnp.where(valid, jnp.exp(masked - largest), 0.0)
        denominator = jnp.sum(raised, axis=-1, keepdims=True) + jnp.exp(sinks - largest)
        weights = (raised / denominator).astype(jnp.bfloat16)
        attended = jnp.einsum(
            "hgqk,khd->qhgd", weights, value_block, preferred_element_type=jnp.float32
        )
        return attended.astype(jnp.bfloat16).reshape(QBLOCK, heads_here * HEAD_DIM)

    attended = lax.map(attend_block, jnp.arange(row_count // QBLOCK, dtype=jnp.int32))
    attended = attended.reshape(row_count, heads_here * HEAD_DIM)
    return lax.all_to_all(attended, "tp", split_axis=0, concat_axis=1, tiled=True)


def project(attended, full_weight, out_gain):
    mixed = jnp.dot(attended, full_weight, preferred_element_type=jnp.float32)
    return (
        mixed * lax.rsqrt(jnp.mean(mixed * mixed, axis=-1, keepdims=True) + epsilon) * out_gain
    ).astype(jnp.bfloat16)


def expert_kernel(x_ref, w_ref, gate_ref, up_ref, down_ref, out_ref, total):
    x = x_ref[...]
    for e in range(gate_ref.shape[0]):
        gate = jnp.dot(x, gate_ref[e], preferred_element_type=jnp.float32)
        upward = jnp.dot(x, up_ref[e], preferred_element_type=jnp.float32)
        hidden = (gate / (1.0 + jnp.exp(-gate)) * upward * w_ref[:, e : e + 1]).astype(
            jnp.bfloat16
        )
        part = lax.dot_general(
            hidden, down_ref[e], (((1,), (1,)), ((), ())), preferred_element_type=jnp.float32
        )
        if e == 0:
            total[...] = part
        else:
            total[...] += part
    out_ref[...] = total[...].astype(jnp.bfloat16)


def apply_experts(rows, weights, gate, up, down):
    count, width = rows.shape
    local_experts, _, units = gate.shape
    tile = min(ROW_TILE, count)
    whole = lambda i: (0, 0, 0)
    return pl.pallas_call(
        expert_kernel,
        grid=(count // tile,),
        out_shape=jax.ShapeDtypeStruct((count, width), jnp.bfloat16),
        in_specs=[
            pl.BlockSpec((tile, width), lambda i: (i, 0)),
            pl.BlockSpec((tile, local_experts), lambda i: (i, 0)),
            pl.BlockSpec(gate.shape, whole, pipeline_mode=pl.Buffered(1)),
            pl.BlockSpec(up.shape, whole, pipeline_mode=pl.Buffered(1)),
            pl.BlockSpec(down.shape, whole, pipeline_mode=pl.Buffered(1)),
        ],
        out_specs=pl.BlockSpec((tile, width), lambda i: (i, 0)),
        scratch_shapes=[pltpu.VMEM((tile, width), jnp.float32)],
        compiler_params=pltpu.CompilerParams(vmem_limit_bytes=48 * 2**20),
        cost_estimate=pl.CostEstimate(
            flops=6 * count * width * local_experts * units,
            bytes_accessed=4 * count * width + 6 * local_experts * units * width,
            transcendentals=count * local_experts * units,
        ),
    )(rows, weights, gate, up, down)


def routed(tokens, expert_ids, route_weight, gain, gate, up, down, full_weight, attended):
    token_total, width = tokens.shape
    share = token_total // GROUPS
    plane = lax.axis_size(PLANE)
    local_experts = gate.shape[0]
    inputs = tokens.astype(jnp.float32)
    normed = (
        inputs * lax.rsqrt(jnp.mean(inputs * inputs, axis=-1, keepdims=True) + epsilon) * gain
    ).astype(jnp.bfloat16)
    group = expert_ids[:, 0] // EPG
    in_group = (group[:, None] == jnp.arange(GROUPS, dtype=jnp.int32)).astype(jnp.float32)
    index = jnp.arange(token_total, dtype=jnp.int32)
    before = (index[None, :] < index[:, None]).astype(jnp.float32)
    ranks = jnp.dot(before, in_group, preferred_element_type=jnp.float32)
    rank = jnp.sum(ranks * in_group, axis=1).astype(jnp.int32)
    position = group * share + rank
    order = (position[None, :] == index[:, None]).astype(jnp.bfloat16)
    back = (position[:, None] == index[None, :]).astype(jnp.bfloat16)
    ordered = jnp.dot(order, normed, preferred_element_type=jnp.float32).astype(jnp.bfloat16)
    member = jnp.arange(EPG, dtype=jnp.int32)
    spread = jnp.sum(
        jnp.where((expert_ids % EPG)[:, :, None] == member, route_weight[:, :, None], 0.0), axis=1
    )
    spread = jnp.dot(
        order.astype(jnp.float32), spread, precision=lax.Precision.HIGHEST,
        preferred_element_type=jnp.float32,
    )
    spread = spread.reshape(GROUPS, share, EPG).transpose(0, 2, 1).reshape(GROUPS, EPG * share)
    spread = lax.all_to_all(spread, "group", 0, 0, tiled=True)
    spread = lax.all_gather(spread, PLANE, axis=0, tiled=True)
    spread = spread.reshape(plane, GROUPS, EPG, share)
    mine = lax.dynamic_slice_in_dim(
        spread, lax.axis_index("member") * local_experts, local_experts, 2
    ).transpose(0, 1, 3, 2)
    piece = max(min(share, CHUNK_ROWS // (plane * GROUPS)), 16)
    ordered = ordered.reshape(GROUPS, share, width)
    mine, attended = lax.optimization_barrier((mine, attended))
    results = []
    for start in range(0, share, piece):
        sent = lax.all_to_all(ordered[:, start : start + piece], "group", 0, 0, tiled=True)
        sent = sent.reshape(GROUPS * piece, width)
        if start == 0:
            sent, full_weight = lax.optimization_barrier((sent, full_weight))
        rows = lax.all_gather(sent, PLANE, axis=0, tiled=True)
        weights = mine[:, :, start : start + piece].reshape(plane * GROUPS * piece, local_experts)
        partial = apply_experts(rows, weights, gate, up, down)
        summed = lax.psum_scatter(partial, PLANE, scatter_dimension=0, tiled=True)
        summed = summed.reshape(GROUPS, piece, width)
        results.append(lax.all_to_all(summed, "group", 0, 0, tiled=True))
    result = jnp.concatenate(results, axis=1).reshape(token_total, width)
    result = jnp.dot(back, result, preferred_element_type=jnp.float32).astype(jnp.bfloat16)
    return result, full_weight, attended


MESH = pl.DeviceIdType.MESH
QUAD = 4
PART_ROWS = 64


def fused_layer(steps, rows, ordered, spread, gate, up, down, queries, pairs, sinks, out_weight,
                out_gain, out, mixer_out,
                xbuf, wraw, wcol, wg, wu, wd, hid, own, part, got1, got2, fin,
                held_queries, band, mine, theirs, wo, mixed, stage,
                send, recv, wsem, ssem, asem):
    plane, member, place = (lax.axis_index(a) for a in ("group", "member", "tp"))
    experts, width, units = gate.shape
    share = spread.shape[-1]
    here = experts * units
    blocks = 2 * experts
    first = rows // 2
    sequence_rows = queries.shape[0]
    heads_here = queries.shape[1] // HEAD_DIM
    lanes = 2 * HEAD_DIM
    token_rows = mixed.shape[0]
    ep_count = GROUPS * 2
    ep_place = plane * 2 + member

    def device(dz=0, dx=0, dy=0, dcore=0):
        z = (plane // 2 + dz // 2) % 2 * 2 + (plane % 2 + dz % 2) % 2
        t = (place // 2 + dx) % 2 * 2 + (place % 2 + dcore) % 2
        return (z, (member + dy) % 2, t)

    def far(s):
        return (s + s // GROUPS) % GROUPS

    def slot(q, start=0, count=rows):
        return pl.ds(pl.multiple_of(q * rows + start, 16), count)

    def remote(src, dst, s, k, target):
        return pltpu.make_async_remote_copy(
            src_ref=src, dst_ref=dst, send_sem=send.at[s, k], recv_sem=recv.at[s, k],
            device_id=target, device_id_type=MESH,
        )

    def tokens_of(s):
        return pl.ds(pl.multiple_of(far(s) * share + s // GROUPS * rows, 16), rows)

    def local_in(s):
        return pltpu.make_async_copy(
            ordered.at[tokens_of(s)], xbuf.at[s, slot(0)], recv.at[s, 0]
        )

    def dispatch(s):
        return remote(ordered.at[tokens_of(s)], xbuf.at[s, slot(0)], s, 0, device(far(s)))

    def to_x(s):
        return remote(xbuf.at[s, slot(0)], xbuf.at[s, slot(1)], s, 1, device(dx=1))

    def to_y(s):
        return remote(xbuf.at[s, slot(0)], xbuf.at[s, slot(2)], s, 2, device(dy=1))

    def pass_y(s):
        return remote(
            xbuf.at[s, slot(1, 0, first)], xbuf.at[s, slot(3, 0, first)], s, 3, device(dy=1)
        )

    def pass_x(s):
        return remote(
            xbuf.at[s, slot(2, first, rows - first)],
            xbuf.at[s, slot(3, first, rows - first)], s, 4, device(dx=1),
        )

    def corner_x(s):
        return remote(
            part.at[s, slot(2, 0, first)], got1.at[s, pl.ds(0, first)], s, 5, device(dx=1)
        )

    def corner_y(s):
        return remote(
            part.at[s, slot(2, first, rows - first)], got1.at[s, pl.ds(first, rows - first)],
            s, 6, device(dy=1),
        )

    def sum_x(s):
        return remote(part.at[s, slot(0)], got2.at[s, slot(0)], s, 7, device(dx=1))

    def sum_y(s):
        return remote(part.at[s, slot(1)], got2.at[s, slot(1)], s, 8, device(dy=1))

    def give_back(s):
        return remote(fin.at[s], out.at[tokens_of(s)], s, 9, device(far(s)))

    def local_out(s):
        return pltpu.make_async_copy(fin.at[s], out.at[tokens_of(s)], recv.at[s, 9])

    def weight_refs(e, to):
        at = to * experts + e
        return (
            (gate.at[e], wg.at[at]),
            (up.at[e], wu.at[at]),
            (down.at[e], wd.at[:, pl.ds(at * units, units)]),
        )

    def weight_copies():
        for e in range(experts):
            for n, (src, dst) in enumerate(weight_refs(e, 0)):
                yield pltpu.make_async_copy(src, dst, wsem.at[0, 3 * e + n])
            for n, (src, dst) in enumerate(weight_refs(e, 1)):
                yield pltpu.make_async_remote_copy(
                    src_ref=src, dst_ref=dst, send_sem=wsem.at[1, 3 * e + n],
                    recv_sem=wsem.at[2, 3 * e + n], device_id=device(dcore=1),
                    device_id_type=MESH,
                )

    def spread_copies():
        for dz in range(GROUPS):
            for q in range(QUAD):
                dx, dy = q % 2, q // 2
                src, dst, n = spread.at[dy, dz], wraw.at[dz, q], dz * QUAD + q
                if n == 0:
                    yield pltpu.make_async_copy(src, dst, ssem.at[1, n])
                else:
                    yield pltpu.make_async_remote_copy(
                        src_ref=src, dst_ref=dst, send_sem=ssem.at[0, n], recv_sem=ssem.at[1, n],
                        device_id=device(dz, dx, dy), device_id_type=MESH,
                    )

    def attention_remote(src, dst, n, target):
        return pltpu.make_async_remote_copy(
            src_ref=src, dst_ref=dst, send_sem=asem.at[0, n], recv_sem=asem.at[1, n],
            device_id=target, device_id_type=MESH,
        )

    def along_ep(distance):
        to = (ep_place + ep_count + distance) % ep_count
        return (to // 2, to % 2, place)

    band_low = attention_remote(
        pairs.at[pl.ds(sequence_rows - WINDOW, WINDOW)], band.at[pl.ds(0, WINDOW)], 0, along_ep(1)
    )
    band_high = attention_remote(
        pairs.at[pl.ds(0, WINDOW)], band.at[pl.ds(WINDOW + sequence_rows, WINDOW)], 1,
        along_ep(-1),
    )
    band_own = pltpu.make_async_copy(pairs, band.at[pl.ds(WINDOW, sequence_rows)], asem.at[2, 0])
    queries_in = pltpu.make_async_copy(queries, held_queries, asem.at[2, 1])
    wo_own = pltpu.make_async_copy(out_weight, wo.at[0], asem.at[2, 2])
    wo_core = attention_remote(out_weight, wo.at[1], 2, device(dcore=1))
    wo_across = attention_remote(out_weight, wo.at[2], 3, device(dx=1))
    wo_pass = attention_remote(wo.at[2], wo.at[3], 4, device(dcore=1))

    def attended_to(k):
        dx, dcore = k // 2, k % 2
        to = device(dx=dx, dcore=dcore)
        start = pl.multiple_of(to[2] * token_rows, 16)
        return attention_remote(
            mine.at[pl.ds(start, token_rows)], theirs.at[k - 1], 4 + k, to
        )

    mixer_done = pltpu.make_async_copy(stage, mixer_out, asem.at[2, 3])

    def attend(b):
        query_rows = WINDOW
        span = 3 * WINDOW
        start = pl.multiple_of(b * query_rows, 16)
        held_band = band[pl.ds(start, span)]
        low = lax.broadcasted_iota(jnp.int32, (span, lanes), 1) < HEAD_DIM
        zero = jnp.zeros((span, lanes), jnp.bfloat16)
        kv, vk = held_band[:, :lanes], held_band[:, lanes:]
        keys = (jnp.where(low, kv, zero), jnp.where(low, zero, vk))
        vals = (jnp.where(low, vk, zero), jnp.where(low, zero, kv))
        row = lax.broadcasted_iota(jnp.int32, (query_rows, span), 0)
        column = lax.broadcasted_iota(jnp.int32, (query_rows, span), 1)
        key_pos = ep_place * sequence_rows + b * query_rows - WINDOW + column
        valid = (
            (column >= row) & (column <= row + 2 * WINDOW)
            & (key_pos >= 0) & (key_pos < ep_count * sequence_rows)
        )
        for pair in range(heads_here // 2):
            query_block = held_queries[
                pl.ds(start, query_rows), pair * lanes : (pair + 1) * lanes
            ]
            total = None
            for side in range(2):
                scores = lax.dot_general(
                    query_block, keys[side], (((1,), (1,)), ((), ())),
                    preferred_element_type=jnp.float32,
                ) * HEAD_DIM ** (-0.5)
                sink = jnp.full((1, 1), sinks[pair * 2 + side], jnp.float32)
                masked = jnp.where(valid, scores, -1e30)
                largest = jnp.maximum(jnp.max(masked, axis=-1, keepdims=True), sink)
                raised = jnp.where(valid, jnp.exp(masked - largest), 0.0)
                denominator = jnp.sum(raised, axis=-1, keepdims=True) + jnp.exp(sink - largest)
                weights = (raised / denominator).astype(jnp.bfloat16)
                product = jnp.dot(weights, vals[side], preferred_element_type=jnp.float32)
                total = product if total is None else total + product
            mine[pl.ds(start, query_rows), pair * lanes : (pair + 1) * lanes] = total.astype(
                jnp.bfloat16
            )

    def project_rows():
        for k in range(1, 4):
            attended_to(k).wait_recv()
        wo_own.wait()
        wo_core.wait_recv()
        wo_pass.wait_recv()
        start = pl.multiple_of(place * token_rows, 16)
        step = 256

        @pl.loop(0, width // step)
        def _(n):
            columns = pl.ds(pl.multiple_of(n * step, step), step)
            total = jnp.dot(
                mine[pl.ds(start, token_rows)], wo[0, :, columns],
                preferred_element_type=jnp.float32,
            )
            for k in range(1, 4):
                total = total + jnp.dot(
                    theirs[k - 1], wo[k, :, columns], preferred_element_type=jnp.float32
                )
            mixed[:, columns] = total

        piece = 32

        @pl.loop(0, token_rows // piece)
        def _(n):
            chosen = pl.ds(pl.multiple_of(n * piece, piece), piece)
            block = mixed[chosen]
            scale = lax.rsqrt(jnp.mean(block * block, axis=-1, keepdims=True) + epsilon)
            stage[chosen] = (block * scale * out_gain[...]).astype(jnp.bfloat16)

        mixer_done.start()

    barrier = pltpu.get_barrier_semaphore()
    peers = [(z, q % 2, q // 2, 0) for z in range(GROUPS) for q in range(QUAD)][1:]
    peers += [(0, 0, 0, 1), (0, 1, 0, 1)]
    for peer in peers:
        pl.semaphore_signal(barrier, inc=1, device_id=device(*peer), device_id_type=MESH)
    pl.semaphore_wait(barrier, len(peers))

    for s in range(steps):
        if far(s) == 0:
            local_in(s).start()
    for s in range(steps):
        if far(s) != 0:
            dispatch(s).start()
    for copy in (band_low, band_high, band_own, queries_in):
        copy.start()
    for copy in spread_copies():
        copy.start()
    for copy in weight_copies():
        copy.start()
    for copy in (wo_own, wo_core, wo_across):
        copy.start()

    def gather(s):
        @pl.when(far(s) == 0)
        def _():
            local_in(s).wait()

        @pl.when(far(s) != 0)
        def _():
            dispatch(s).wait_recv()

        to_x(s).start()
        to_y(s).start()

    def forward(s):
        to_x(s).wait_recv()
        pass_y(s).start()
        to_y(s).wait_recv()
        pass_x(s).start()

    gather(0)
    band_own.wait()
    queries_in.wait()
    band_low.wait_recv()
    band_high.wait_recv()
    blocks_here = sequence_rows // WINDOW
    turns = (blocks_here // 4, blocks_here * 5 // 8)

    @pl.loop(0, blocks_here)
    def _(b):
        @pl.when(b == turns[0])
        def _():
            forward(0)
            gather(1)

        @pl.when(b == turns[1])
        def _():
            forward(1)
            gather(2)

        attend(b)

    for k in range(1, 4):
        attended_to(k).start()
    wo_across.wait_recv()
    wo_pass.start()

    for copy in spread_copies():
        if hasattr(copy, "wait_recv") and copy.is_remote:
            copy.wait_recv()
        else:
            copy.wait()
    for dz in range(GROUPS):
        for q in range(QUAD):
            turned = wraw[dz, q].T
            for piece in range(share // rows):
                s = piece * GROUPS + (dz - piece) % GROUPS
                wcol[s, q * rows : (q + 1) * rows, :] = turned[piece * rows : (piece + 1) * rows]
    for copy in weight_copies():
        if copy.is_remote:
            copy.wait_recv()
        else:
            copy.wait()

    def compute(s):
        for j in range(blocks):
            x = xbuf[s]
            g = jnp.dot(x, wg[j], preferred_element_type=jnp.float32)
            u = jnp.dot(x, wu[j], preferred_element_type=jnp.float32)
            e = j % experts
            h = g / (1.0 + jnp.exp(-g)) * u * wcol[s, :, e : e + 1]
            hid[:, j * units : (j + 1) * units] = h.astype(jnp.bfloat16)
        step = 256

        @pl.loop(0, width // step)
        def _(n):
            columns = pl.ds(pl.multiple_of(n * step, step), step)
            p = lax.dot_general(
                hid[...], wd[columns, :], (((1,), (1,)), ((), ())),
                preferred_element_type=jnp.float32,
            )
            own[s % 3, :, columns] = p[:rows]
            part[s, :, columns] = p[rows:].astype(jnp.bfloat16)

    def settle(s):
        corner_x(s).wait_recv()
        held = part[s, rows : rows + first].astype(jnp.float32)
        part[s, rows : rows + first] = (
            held + got1[s, :first].astype(jnp.float32)
        ).astype(jnp.bfloat16)
        sum_y(s).start()
        corner_y(s).wait_recv()
        held = part[s, first:rows].astype(jnp.float32)
        part[s, first:rows] = (held + got1[s, first:].astype(jnp.float32)).astype(jnp.bfloat16)
        sum_x(s).start()

    def finish(s):
        sum_y(s).wait_recv()
        sum_x(s).wait_recv()
        fin[s] = (
            own[s % 3] + got2[s, :rows].astype(jnp.float32) + got2[s, rows:].astype(jnp.float32)
        ).astype(jnp.bfloat16)

        @pl.when(far(s) == 0)
        def _():
            local_out(s).start()

        @pl.when(far(s) != 0)
        def _():
            give_back(s).start()

    @pl.loop(0, steps + 2)
    def _(i):
        @pl.when(i + 2 < steps)
        def _():
            forward(i + 2)

        @pl.when(i + 3 < steps)
        def _():
            gather(i + 3)

        @pl.when(i >= 2)
        def _():
            finish(i - 2)

        @pl.when(i < steps)
        def _():
            pass_y(i).wait_recv()
            pass_x(i).wait_recv()
            compute(i)
            corner_x(i).start()
            corner_y(i).start()

        @pl.when(jnp.logical_and(i >= 1, i < steps + 1))
        def _():
            settle(i - 1)

        @pl.when(i == steps // 2)
        def _():
            project_rows()

    mixer_done.wait()
    for k in range(1, 4):
        attended_to(k).wait_send()
    for copy in (band_low, band_high, wo_core, wo_across, wo_pass):
        copy.wait_send()
    for copy in spread_copies():
        if copy.is_remote:
            copy.wait_send()
    for copy in weight_copies():
        if copy.is_remote:
            copy.wait_send()

    @pl.loop(0, steps)
    def _(s):
        for copy in (to_x, to_y, pass_y, pass_x, corner_x, corner_y, sum_x, sum_y):
            copy(s).wait_send()

        @pl.when(far(s) == 0)
        def _():
            local_out(s).wait()

        @pl.when(far(s) != 0)
        def _():
            dispatch(s).wait_send()
            give_back(s).wait()


def apply_fused(ordered, spread, gate, up, down, queries, pairs, sinks, out_weight, out_gain):
    total, width = ordered.shape
    experts, _, units = gate.shape
    share = total // GROUPS
    rows = min(PART_ROWS, share)
    steps = total // rows
    hidden = 2 * experts * units
    sequence_rows, head_columns = queries.shape
    token_rows = sequence_rows // 4
    anywhere = pl.BlockSpec(memory_space=pl.ANY)
    vector = pl.BlockSpec(memory_space=pltpu.VMEM)
    scalar = pl.BlockSpec(memory_space=pltpu.SMEM)
    dma = pltpu.SemaphoreType.DMA
    return pl.pallas_call(
        functools.partial(fused_layer, steps, rows),
        out_shape=(
            jax.ShapeDtypeStruct((total, width), jnp.bfloat16),
            jax.ShapeDtypeStruct((token_rows, width), jnp.bfloat16),
        ),
        in_specs=[anywhere] * 7 + [scalar, anywhere, vector],
        out_specs=(anywhere, anywhere),
        scratch_shapes=[
            pltpu.VMEM((steps, QUAD * rows, width), jnp.bfloat16),
            pltpu.VMEM((GROUPS, QUAD) + spread.shape[-2:], jnp.float32),
            pltpu.VMEM((steps, QUAD * rows, EPG), jnp.float32),
            pltpu.VMEM((2 * experts, width, units), jnp.bfloat16),
            pltpu.VMEM((2 * experts, width, units), jnp.bfloat16),
            pltpu.VMEM((width, hidden), jnp.bfloat16),
            pltpu.VMEM((QUAD * rows, hidden), jnp.bfloat16),
            pltpu.VMEM((3, rows, width), jnp.float32),
            pltpu.VMEM((steps, (QUAD - 1) * rows, width), jnp.bfloat16),
            pltpu.VMEM((steps, rows, width), jnp.bfloat16),
            pltpu.VMEM((steps, 2 * rows, width), jnp.bfloat16),
            pltpu.VMEM((steps, rows, width), jnp.bfloat16),
            pltpu.VMEM(queries.shape, jnp.bfloat16),
            pltpu.VMEM((sequence_rows + 2 * WINDOW, pairs.shape[1]), jnp.bfloat16),
            pltpu.VMEM(queries.shape, jnp.bfloat16),
            pltpu.VMEM((3, token_rows, head_columns), jnp.bfloat16),
            pltpu.VMEM((4,) + out_weight.shape, jnp.bfloat16),
            pltpu.VMEM((token_rows, width), jnp.float32),
            pltpu.VMEM((token_rows, width), jnp.bfloat16),
            dma((steps, 10)),
            dma((steps, 10)),
            dma((3, 3 * experts)),
            dma((2, GROUPS * QUAD)),
            dma((3, 8)),
        ],
        compiler_params=pltpu.CompilerParams(
            collective_id=0, has_side_effects=True, vmem_limit_bytes=66 * 10**6
        ),
        cost_estimate=pl.CostEstimate(
            flops=6 * QUAD * total * width * hidden,
            bytes_accessed=6 * experts * units * width,
            transcendentals=QUAD * total * hidden,
        ),
    )(ordered, spread, gate, up, down, queries, pairs, sinks, out_weight, out_gain)


def layer_fused(queries, key_rows, values, sink_logit, out_weight, out_gain, tokens, expert_ids,
                route_weight, gain, gate, up, down):
    token_total, width = tokens.shape
    share = token_total // GROUPS
    local_experts = gate.shape[0]
    inputs = tokens.astype(jnp.float32)
    normed = (
        inputs * lax.rsqrt(jnp.mean(inputs * inputs, axis=-1, keepdims=True) + epsilon) * gain
    ).astype(jnp.bfloat16)
    group = jnp.bitwise_xor(expert_ids[:, 0] // EPG, lax.axis_index("group"))
    in_group = (group[:, None] == jnp.arange(GROUPS, dtype=jnp.int32)).astype(jnp.float32)
    index = jnp.arange(token_total, dtype=jnp.int32)
    before = (index[None, :] < index[:, None]).astype(jnp.float32)
    ranks = jnp.dot(before, in_group, preferred_element_type=jnp.float32)
    rank = jnp.sum(ranks * in_group, axis=1).astype(jnp.int32)
    position = group * share + rank
    order = (position[None, :] == index[:, None]).astype(jnp.bfloat16)
    back = (position[:, None] == index[None, :]).astype(jnp.bfloat16)
    ordered = jnp.dot(order, normed, preferred_element_type=jnp.float32).astype(jnp.bfloat16)
    start = lax.axis_index("member") * local_experts
    member = (jnp.arange(EPG, dtype=jnp.int32) + start) % EPG
    spread = jnp.sum(
        jnp.where((expert_ids % EPG)[:, :, None] == member, route_weight[:, :, None], 0.0), axis=1
    )
    spread = jnp.dot(
        order.astype(jnp.float32), spread, precision=lax.Precision.HIGHEST,
        preferred_element_type=jnp.float32,
    )
    spread = spread.reshape(GROUPS, share, EPG).transpose(0, 2, 1)
    spread = jnp.stack([spread, jnp.roll(spread, local_experts, axis=1)])
    pairs = jnp.concatenate([key_rows, values, values, key_rows], axis=1)
    result, mixer_out = apply_fused(
        ordered, spread, gate, up, down, queries, pairs, sink_logit, out_weight,
        out_gain.reshape(1, width),
    )
    result = jnp.dot(back, result, preferred_element_type=jnp.float32).astype(jnp.bfloat16)
    return (mixer_out, result)


def can_fuse(queries, key_rows):
    return (
        lax.axis_size("group") == GROUPS
        and lax.axis_size("member") == 2
        and lax.axis_size("tp") == 4
        and key_rows.shape[1] == HEAD_DIM
        and queries.shape[1] % (2 * HEAD_DIM) == 0
    )


def local(queries, key_rows, values, sink_logit, out_weight, out_gain, routed_tokens,
          expert_ids, route_weight, routed_gain, expert_gate, expert_up, expert_down):
    if can_fuse(queries, key_rows):
        return layer_fused(
            queries, key_rows, values, sink_logit, out_weight, out_gain, routed_tokens,
            expert_ids, route_weight, routed_gain, expert_gate, expert_up, expert_down,
        )
    full_weight = lax.all_gather(out_weight, "tp", axis=0, tiled=True)
    attended = attention(queries, key_rows, values, sink_logit)
    experts_out, full_weight, attended = routed(
        routed_tokens, expert_ids, route_weight, routed_gain, expert_gate, expert_up, expert_down,
        full_weight, attended,
    )
    mixer_out = project(attended, full_weight, out_gain)
    return (mixer_out, experts_out)


def solution(mesh):
    ep, tp = mesh.shape["ep"], mesh.shape["tp"]
    split = Mesh(mesh.devices.reshape(GROUPS, ep // GROUPS, tp), ("group", "member", "tp"))
    every = ("group", "member", "tp")
    placed = (
        P(EP, "tp"),
        P(EP, "tp"),
        P(EP, "tp"),
        P("tp"),
        P("tp", None),
        P(),
        P(every, None),
        P(every, None),
        P(every, None),
        P(),
        P(EP, None, "tp"),
        P(EP, None, "tp"),
        P(EP, None, "tp"),
    )
    return jax.shard_map(
        local,
        mesh=split,
        in_specs=placed,
        out_specs=(P(every, None), P(every, None)),
        check_vma=False,
    )
```

```python
import functools

import jax
import jax.numpy as jnp
from jax import lax
from jax.experimental import pallas as pl
from jax.experimental.pallas import tpu as pltpu
from jax.sharding import Mesh, PartitionSpec as P

HEAD_DIM = 64
WINDOW = 128
QBLOCK = 512
EXPERTS = 32
EPG = 8
TOP = 2
GROUPS = EXPERTS // EPG
CHUNK_ROWS = 2048
ROW_TILE = 512

epsilon = 1e-06
EP = ("group", "member")
PLANE = ("member", "tp")


def padded(block, width):
    count = lax.axis_size(EP)
    forward = [(i, i + 1) for i in range(count - 1)]
    backward = [(target, source) for source, target in forward]
    low = lax.ppermute(block[-width:], EP, forward)
    high = lax.ppermute(block[:width], EP, backward)
    return jnp.concatenate([low, block, high], axis=0)


def attention(queries, key_rows, values, sink_logit):
    row_count = queries.shape[0]
    heads_here = queries.shape[1] // HEAD_DIM
    kv_here = key_rows.shape[1] // HEAD_DIM
    group_size = heads_here // kv_here
    paired = jnp.concatenate((key_rows, values), axis=1)
    extended = padded(paired, WINDOW)
    offset = lax.axis_index(EP) * row_count
    seq_total = row_count * lax.axis_size(EP)
    grouped = queries.reshape(row_count, kv_here, group_size, HEAD_DIM)
    sinks = sink_logit.reshape(kv_here, group_size)[:, :, None, None]
    span_keys = QBLOCK + 2 * WINDOW

    def attend_block(block_index):
        start_row = block_index * QBLOCK
        query_block = lax.dynamic_slice_in_dim(grouped, start_row, QBLOCK, 0)
        band = lax.dynamic_slice_in_dim(extended, start_row, span_keys, 0)
        key_block = band[:, : kv_here * HEAD_DIM].reshape(span_keys, kv_here, HEAD_DIM)
        value_block = band[:, kv_here * HEAD_DIM :].reshape(span_keys, kv_here, HEAD_DIM)
        scores = jnp.einsum(
            "qhgd,khd->hgqk", query_block, key_block, preferred_element_type=jnp.float32
        ) * HEAD_DIM ** (-0.5)
        query_pos = offset + start_row + jnp.arange(QBLOCK, dtype=jnp.int32)
        key_pos = offset + start_row - WINDOW + jnp.arange(span_keys, dtype=jnp.int32)
        valid = (
            (jnp.abs(key_pos[None, :] - query_pos[:, None]) <= WINDOW)
            & (key_pos[None, :] >= 0)
            & (key_pos[None, :] < seq_total)
        )
        masked = jnp.where(valid, scores, -1e30)
        largest = jnp.maximum(jnp.max(masked, axis=-1, keepdims=True), sinks)
        raised = jnp.where(valid, jnp.exp(masked - largest), 0.0)
        denominator = jnp.sum(raised, axis=-1, keepdims=True) + jnp.exp(sinks - largest)
        weights = (raised / denominator).astype(jnp.bfloat16)
        attended = jnp.einsum(
            "hgqk,khd->qhgd", weights, value_block, preferred_element_type=jnp.float32
        )
        return attended.astype(jnp.bfloat16).reshape(QBLOCK, heads_here * HEAD_DIM)

    attended = lax.map(attend_block, jnp.arange(row_count // QBLOCK, dtype=jnp.int32))
    attended = attended.reshape(row_count, heads_here * HEAD_DIM)
    return lax.all_to_all(attended, "tp", split_axis=0, concat_axis=1, tiled=True)


def project(attended, full_weight, out_gain):
    mixed = jnp.dot(attended, full_weight, preferred_element_type=jnp.float32)
    return (
        mixed * lax.rsqrt(jnp.mean(mixed * mixed, axis=-1, keepdims=True) + epsilon) * out_gain
    ).astype(jnp.bfloat16)


def expert_kernel(x_ref, w_ref, gate_ref, up_ref, down_ref, out_ref, total):
    x = x_ref[...]
    for e in range(gate_ref.shape[0]):
        gate = jnp.dot(x, gate_ref[e], preferred_element_type=jnp.float32)
        upward = jnp.dot(x, up_ref[e], preferred_element_type=jnp.float32)
        hidden = (gate / (1.0 + jnp.exp(-gate)) * upward * w_ref[:, e : e + 1]).astype(
            jnp.bfloat16
        )
        part = lax.dot_general(
            hidden, down_ref[e], (((1,), (1,)), ((), ())), preferred_element_type=jnp.float32
        )
        if e == 0:
            total[...] = part
        else:
            total[...] += part
    out_ref[...] = total[...].astype(jnp.bfloat16)


def apply_experts(rows, weights, gate, up, down):
    count, width = rows.shape
    local_experts, _, units = gate.shape
    tile = min(ROW_TILE, count)
    whole = lambda i: (0, 0, 0)
    return pl.pallas_call(
        expert_kernel,
        grid=(count // tile,),
        out_shape=jax.ShapeDtypeStruct((count, width), jnp.bfloat16),
        in_specs=[
            pl.BlockSpec((tile, width), lambda i: (i, 0)),
            pl.BlockSpec((tile, local_experts), lambda i: (i, 0)),
            pl.BlockSpec(gate.shape, whole, pipeline_mode=pl.Buffered(1)),
            pl.BlockSpec(up.shape, whole, pipeline_mode=pl.Buffered(1)),
            pl.BlockSpec(down.shape, whole, pipeline_mode=pl.Buffered(1)),
        ],
        out_specs=pl.BlockSpec((tile, width), lambda i: (i, 0)),
        scratch_shapes=[pltpu.VMEM((tile, width), jnp.float32)],
        compiler_params=pltpu.CompilerParams(vmem_limit_bytes=48 * 2**20),
        cost_estimate=pl.CostEstimate(
            flops=6 * count * width * local_experts * units,
            bytes_accessed=4 * count * width + 6 * local_experts * units * width,
            transcendentals=count * local_experts * units,
        ),
    )(rows, weights, gate, up, down)


def routed(tokens, expert_ids, route_weight, gain, gate, up, down, full_weight, attended):
    token_total, width = tokens.shape
    share = token_total // GROUPS
    plane = lax.axis_size(PLANE)
    local_experts = gate.shape[0]
    inputs = tokens.astype(jnp.float32)
    normed = (
        inputs * lax.rsqrt(jnp.mean(inputs * inputs, axis=-1, keepdims=True) + epsilon) * gain
    ).astype(jnp.bfloat16)
    group = expert_ids[:, 0] // EPG
    in_group = (group[:, None] == jnp.arange(GROUPS, dtype=jnp.int32)).astype(jnp.float32)
    index = jnp.arange(token_total, dtype=jnp.int32)
    before = (index[None, :] < index[:, None]).astype(jnp.float32)
    ranks = jnp.dot(before, in_group, preferred_element_type=jnp.float32)
    rank = jnp.sum(ranks * in_group, axis=1).astype(jnp.int32)
    position = group * share + rank
    order = (position[None, :] == index[:, None]).astype(jnp.bfloat16)
    back = (position[:, None] == index[None, :]).astype(jnp.bfloat16)
    ordered = jnp.dot(order, normed, preferred_element_type=jnp.float32).astype(jnp.bfloat16)
    member = jnp.arange(EPG, dtype=jnp.int32)
    spread = jnp.sum(
        jnp.where((expert_ids % EPG)[:, :, None] == member, route_weight[:, :, None], 0.0), axis=1
    )
    spread = jnp.dot(
        order.astype(jnp.float32), spread, precision=lax.Precision.HIGHEST,
        preferred_element_type=jnp.float32,
    )
    spread = spread.reshape(GROUPS, share, EPG).transpose(0, 2, 1).reshape(GROUPS, EPG * share)
    spread = lax.all_to_all(spread, "group", 0, 0, tiled=True)
    spread = lax.all_gather(spread, PLANE, axis=0, tiled=True)
    spread = spread.reshape(plane, GROUPS, EPG, share)
    mine = lax.dynamic_slice_in_dim(
        spread, lax.axis_index("member") * local_experts, local_experts, 2
    ).transpose(0, 1, 3, 2)
    piece = max(min(share, CHUNK_ROWS // (plane * GROUPS)), 16)
    ordered = ordered.reshape(GROUPS, share, width)
    mine, attended = lax.optimization_barrier((mine, attended))
    results = []
    for start in range(0, share, piece):
        sent = lax.all_to_all(ordered[:, start : start + piece], "group", 0, 0, tiled=True)
        sent = sent.reshape(GROUPS * piece, width)
        if start == 0:
            sent, full_weight = lax.optimization_barrier((sent, full_weight))
        rows = lax.all_gather(sent, PLANE, axis=0, tiled=True)
        weights = mine[:, :, start : start + piece].reshape(plane * GROUPS * piece, local_experts)
        partial = apply_experts(rows, weights, gate, up, down)
        summed = lax.psum_scatter(partial, PLANE, scatter_dimension=0, tiled=True)
        summed = summed.reshape(GROUPS, piece, width)
        results.append(lax.all_to_all(summed, "group", 0, 0, tiled=True))
    result = jnp.concatenate(results, axis=1).reshape(token_total, width)
    result = jnp.dot(back, result, preferred_element_type=jnp.float32).astype(jnp.bfloat16)
    return result, full_weight, attended


MESH = pl.DeviceIdType.MESH
QUAD = 4
PART_ROWS = 64
LAG = 3
DEPTH = 1


def fused_layer(steps, rows, ordered, spread, gate, up, down, queries, pairs, sinks, out_weight,
                out_gain, out, mixer_out,
                xbuf, wraw, wcol, wg, wu, wd, hid, own, part, got1, got2, fin,
                held_queries, band, mine, theirs, wo, mixed, stage,
                send, recv, wsem, ssem, asem, wosem):
    plane, member, place = (lax.axis_index(a) for a in ("group", "member", "tp"))
    experts, width, units = gate.shape
    share = spread.shape[-1]
    here = experts * units
    blocks = 2 * experts
    first = rows // 2
    early = rows * 3 // 4 // 16 * 16
    wo_rows = out_weight.shape[0] // steps
    sequence_rows = queries.shape[0]
    heads_here = queries.shape[1] // HEAD_DIM
    lanes = 2 * HEAD_DIM
    token_rows = mixed.shape[0]
    ep_count = GROUPS * 2
    ep_place = plane * 2 + member

    def device(dz=0, dx=0, dy=0, dcore=0):
        z = (plane // 2 + dz // 2) % 2 * 2 + (plane % 2 + dz % 2) % 2
        t = (place // 2 + dx) % 2 * 2 + (place % 2 + dcore) % 2
        return (z, (member + dy) % 2, t)

    def far(s):
        return (s + s // GROUPS) % GROUPS

    def slot(q, start=0, count=rows):
        return pl.ds(pl.multiple_of(q * rows + start, 16), count)

    def remote(src, dst, s, k, target):
        return pltpu.make_async_remote_copy(
            src_ref=src, dst_ref=dst, send_sem=send.at[s, k], recv_sem=recv.at[s, k],
            device_id=target, device_id_type=MESH,
        )

    def tokens_of(s):
        return pl.ds(pl.multiple_of(far(s) * share + s // GROUPS * rows, 16), rows)

    def local_in(s):
        return pltpu.make_async_copy(
            ordered.at[tokens_of(s)], xbuf.at[s, slot(0)], recv.at[s, 0]
        )

    def dispatch(s):
        return remote(ordered.at[tokens_of(s)], xbuf.at[s, slot(0)], s, 0, device(far(s)))

    def to_x(s):
        return remote(xbuf.at[s, slot(0)], xbuf.at[s, slot(1)], s, 1, device(dx=1))

    def to_y(s):
        return remote(xbuf.at[s, slot(0)], xbuf.at[s, slot(2)], s, 2, device(dy=1))

    def pass_y(s):
        return remote(
            xbuf.at[s, slot(1, 0, early)], xbuf.at[s, slot(3, 0, early)], s, 3, device(dy=1)
        )

    def pass_x(s):
        return remote(
            xbuf.at[s, slot(2, early, rows - early)],
            xbuf.at[s, slot(3, early, rows - early)], s, 4, device(dx=1),
        )

    def corner_x(s):
        return remote(
            part.at[s, slot(2, 0, first)], got1.at[s, pl.ds(0, first)], s, 5, device(dx=1)
        )

    def corner_y(s):
        return remote(
            part.at[s, slot(2, first, rows - first)], got1.at[s, pl.ds(first, rows - first)],
            s, 6, device(dy=1),
        )

    def sum_x(s):
        return remote(part.at[s, slot(0)], got2.at[s, slot(0)], s, 7, device(dx=1))

    def sum_y(s):
        return remote(part.at[s, slot(1)], got2.at[s, slot(1)], s, 8, device(dy=1))

    def give_back(s):
        return remote(fin.at[s], out.at[tokens_of(s)], s, 9, device(far(s)))

    def local_out(s):
        return pltpu.make_async_copy(fin.at[s], out.at[tokens_of(s)], recv.at[s, 9])

    def weight_refs(e, to):
        at = to * experts + e
        return (
            (gate.at[e], wg.at[at]),
            (up.at[e], wu.at[at]),
            (down.at[e], wd.at[:, pl.ds(at * units, units)]),
        )

    def weight_copies():
        for e in range(experts):
            for n, (src, dst) in enumerate(weight_refs(e, 0)):
                yield pltpu.make_async_copy(src, dst, wsem.at[0, 3 * e + n])
            for n, (src, dst) in enumerate(weight_refs(e, 1)):
                yield pltpu.make_async_remote_copy(
                    src_ref=src, dst_ref=dst, send_sem=wsem.at[1, 3 * e + n],
                    recv_sem=wsem.at[2, 3 * e + n], device_id=device(dcore=1),
                    device_id_type=MESH,
                )

    def spread_copies():
        for dz in range(GROUPS):
            for q in range(QUAD):
                dx, dy = q % 2, q // 2
                src, dst, n = spread.at[dy, dz], wraw.at[dz, q], dz * QUAD + q
                if n == 0:
                    yield pltpu.make_async_copy(src, dst, ssem.at[1, n])
                else:
                    yield pltpu.make_async_remote_copy(
                        src_ref=src, dst_ref=dst, send_sem=ssem.at[0, n], recv_sem=ssem.at[1, n],
                        device_id=device(dz, dx, dy), device_id_type=MESH,
                    )

    def attention_remote(src, dst, n, target):
        return pltpu.make_async_remote_copy(
            src_ref=src, dst_ref=dst, send_sem=asem.at[0, n], recv_sem=asem.at[1, n],
            device_id=target, device_id_type=MESH,
        )

    def along_ep(distance):
        to = (ep_place + ep_count + distance) % ep_count
        return (to // 2, to % 2, place)

    band_low = attention_remote(
        pairs.at[pl.ds(sequence_rows - WINDOW, WINDOW)], band.at[pl.ds(0, WINDOW)], 0, along_ep(1)
    )
    band_high = attention_remote(
        pairs.at[pl.ds(0, WINDOW)], band.at[pl.ds(WINDOW + sequence_rows, WINDOW)], 1,
        along_ep(-1),
    )
    band_own = pltpu.make_async_copy(pairs, band.at[pl.ds(WINDOW, sequence_rows)], asem.at[2, 0])
    queries_in = pltpu.make_async_copy(queries, held_queries, asem.at[2, 1])
    wo_own = pltpu.make_async_copy(out_weight, wo.at[0], asem.at[2, 2])
    wo_core = attention_remote(out_weight, wo.at[1], 2, device(dcore=1))

    def wo_piece(src, k, n, target):
        piece = pl.ds(pl.multiple_of(n * wo_rows, 16), wo_rows)
        return pltpu.make_async_remote_copy(
            src_ref=src.at[piece], dst_ref=wo.at[k, piece], send_sem=wosem.at[k - 2, n],
            recv_sem=wosem.at[k, n], device_id=target, device_id_type=MESH,
        )

    def wo_across(n):
        return wo_piece(out_weight, 2, n, device(dx=1))

    def wo_pass(n):
        return wo_piece(wo.at[2], 3, n, device(dcore=1))

    def attended_to(k):
        dx, dcore = k // 2, k % 2
        to = device(dx=dx, dcore=dcore)
        start = pl.multiple_of(to[2] * token_rows, 16)
        return attention_remote(
            mine.at[pl.ds(start, token_rows)], theirs.at[k - 1], 4 + k, to
        )

    mixer_done = pltpu.make_async_copy(stage, mixer_out, asem.at[2, 3])

    def attend(b):
        query_rows = WINDOW
        span = 3 * WINDOW
        start = pl.multiple_of(b * query_rows, 16)
        held_band = band[pl.ds(start, span)]
        low = lax.broadcasted_iota(jnp.int32, (span, lanes), 1) < HEAD_DIM
        zero = jnp.zeros((span, lanes), jnp.bfloat16)
        kv, vk = held_band[:, :lanes], held_band[:, lanes:]
        keys = (jnp.where(low, kv, zero), jnp.where(low, zero, vk))
        vals = (jnp.where(low, vk, zero), jnp.where(low, zero, kv))
        row = lax.broadcasted_iota(jnp.int32, (query_rows, span), 0)
        column = lax.broadcasted_iota(jnp.int32, (query_rows, span), 1)
        key_pos = ep_place * sequence_rows + b * query_rows - WINDOW + column
        valid = (
            (column >= row) & (column <= row + 2 * WINDOW)
            & (key_pos >= 0) & (key_pos < ep_count * sequence_rows)
        )
        for pair in range(heads_here // 2):
            query_block = held_queries[
                pl.ds(start, query_rows), pair * lanes : (pair + 1) * lanes
            ]
            total = None
            for side in range(2):
                scores = lax.dot_general(
                    query_block, keys[side], (((1,), (1,)), ((), ())),
                    preferred_element_type=jnp.float32,
                ) * HEAD_DIM ** (-0.5)
                sink = jnp.full((1, 1), sinks[pair * 2 + side], jnp.float32)
                masked = jnp.where(valid, scores, -1e30)
                largest = jnp.maximum(jnp.max(masked, axis=-1, keepdims=True), sink)
                raised = jnp.where(valid, jnp.exp(masked - largest), 0.0)
                denominator = jnp.sum(raised, axis=-1, keepdims=True) + jnp.exp(sink - largest)
                weights = (raised / denominator).astype(jnp.bfloat16)
                product = jnp.dot(weights, vals[side], preferred_element_type=jnp.float32)
                total = product if total is None else total + product
            mine[pl.ds(start, query_rows), pair * lanes : (pair + 1) * lanes] = total.astype(
                jnp.bfloat16
            )

    def project_rows():
        for k in range(1, 4):
            attended_to(k).wait_recv()
        wo_own.wait()
        wo_core.wait_recv()

        @pl.loop(0, steps)
        def _(n):
            wo_pass(n).wait_recv()

        start = pl.multiple_of(place * token_rows, 16)
        step = 256

        @pl.loop(0, width // step)
        def _(n):
            columns = pl.ds(pl.multiple_of(n * step, step), step)
            total = jnp.dot(
                mine[pl.ds(start, token_rows)], wo[0, :, columns],
                preferred_element_type=jnp.float32,
            )
            for k in range(1, 4):
                total = total + jnp.dot(
                    theirs[k - 1], wo[k, :, columns], preferred_element_type=jnp.float32
                )
            mixed[:, columns] = total

        piece = 32

        @pl.loop(0, token_rows // piece)
        def _(n):
            chosen = pl.ds(pl.multiple_of(n * piece, piece), piece)
            block = mixed[chosen]
            scale = lax.rsqrt(jnp.mean(block * block, axis=-1, keepdims=True) + epsilon)
            stage[chosen] = (block * scale * out_gain[...]).astype(jnp.bfloat16)

        mixer_done.start()

    barrier = pltpu.get_barrier_semaphore()
    peers = [(z, q % 2, q // 2, 0) for z in range(GROUPS) for q in range(QUAD)][1:]
    peers += [(0, 0, 0, 1), (0, 1, 0, 1)]
    for peer in peers:
        pl.semaphore_signal(barrier, inc=1, device_id=device(*peer), device_id_type=MESH)
    pl.semaphore_wait(barrier, len(peers))

    for s in range(steps):
        if far(s) == 0:
            local_in(s).start()
    def gather(s):
        @pl.when(far(s) == 0)
        def _():
            local_in(s).wait()

        @pl.when(far(s) != 0)
        def _():
            dispatch(s).wait_recv()

        to_x(s).start()
        to_y(s).start()
        more = s + DEPTH

        @pl.when(jnp.logical_and(more < steps, far(more) != 0))
        def _():
            dispatch(more).start()

    def forward(s):
        to_x(s).wait_recv()
        pass_y(s).start()
        to_y(s).wait_recv()
        pass_x(s).start()

    for s in range(1, DEPTH):
        if far(s) != 0:
            dispatch(s).start()
    gather(0)
    for copy in (band_low, band_high, band_own, queries_in):
        copy.start()
    for copy in spread_copies():
        copy.start()
    for copy in weight_copies():
        copy.start()
    for copy in (wo_own, wo_core):
        copy.start()
    wo_across(0).start()
    wo_across(1).start()
    band_own.wait()
    queries_in.wait()
    band_low.wait_recv()
    band_high.wait_recv()
    blocks_here = sequence_rows // WINDOW
    turns = (blocks_here // 4, blocks_here * 5 // 8)

    @pl.loop(0, blocks_here)
    def _(b):
        @pl.when(b == turns[0])
        def _():
            forward(0)
            gather(1)

        @pl.when(b == turns[1])
        def _():
            forward(1)
            gather(2)

        attend(b)

    for k in range(1, 4):
        attended_to(k).start()

    for copy in spread_copies():
        if hasattr(copy, "wait_recv") and copy.is_remote:
            copy.wait_recv()
        else:
            copy.wait()
    for dz in range(GROUPS):
        for q in range(QUAD):
            turned = wraw[dz, q].T
            for piece in range(share // rows):
                s = piece * GROUPS + (dz - piece) % GROUPS
                wcol[s, q * rows : (q + 1) * rows, :] = turned[piece * rows : (piece + 1) * rows]
    for copy in weight_copies():
        if copy.is_remote:
            copy.wait_recv()
        else:
            copy.wait()

    def compute(s):
        for j in range(blocks):
            x = xbuf[s]
            g = jnp.dot(x, wg[j], preferred_element_type=jnp.float32)
            u = jnp.dot(x, wu[j], preferred_element_type=jnp.float32)
            e = j % experts
            h = g / (1.0 + jnp.exp(-g)) * u * wcol[s, :, e : e + 1]
            hid[:, j * units : (j + 1) * units] = h.astype(jnp.bfloat16)
        step = 256

        @pl.loop(0, width // step)
        def _(n):
            columns = pl.ds(pl.multiple_of(n * step, step), step)
            p = lax.dot_general(
                hid[...], wd[columns, :], (((1,), (1,)), ((), ())),
                preferred_element_type=jnp.float32,
            )
            own[s % LAG, :, columns] = p[:rows]
            part[s, :, columns] = p[rows:].astype(jnp.bfloat16)

    def settle(s):
        corner_x(s).wait_recv()
        held = part[s, rows : rows + first].astype(jnp.float32)
        part[s, rows : rows + first] = (
            held + got1[s, :first].astype(jnp.float32)
        ).astype(jnp.bfloat16)
        sum_y(s).start()
        corner_y(s).wait_recv()
        held = part[s, first:rows].astype(jnp.float32)
        part[s, first:rows] = (held + got1[s, first:].astype(jnp.float32)).astype(jnp.bfloat16)
        sum_x(s).start()

    def finish(s):
        sum_y(s).wait_recv()
        sum_x(s).wait_recv()
        fin[s] = (
            own[s % LAG] + got2[s, :rows].astype(jnp.float32) + got2[s, rows:].astype(jnp.float32)
        ).astype(jnp.bfloat16)

        @pl.when(far(s) == 0)
        def _():
            local_out(s).start()

        @pl.when(far(s) != 0)
        def _():
            give_back(s).start()

    @pl.loop(0, steps + LAG - 1)
    def _(i):
        @pl.when(i + 2 < steps)
        def _():
            forward(i + 2)
            wo_across(i + 2).start()

        @pl.when(i + 3 < steps)
        def _():
            gather(i + 3)

        @pl.when(jnp.logical_and(i >= 1, i <= steps))
        def _():
            wo_across(i - 1).wait_recv()
            wo_pass(i - 1).start()

        @pl.when(i < steps)
        def _():
            pass_y(i).wait_recv()
            pass_x(i).wait_recv()
            compute(i)
            corner_x(i).start()
            corner_y(i).start()

        @pl.when(jnp.logical_and(i >= 1, i <= steps))
        def _():
            settle(i - 1)

        @pl.when(i >= LAG - 1)
        def _():
            finish(i - LAG + 1)

        @pl.when(i == steps)
        def _():
            project_rows()

    mixer_done.wait()
    for k in range(1, 4):
        attended_to(k).wait_send()
    for copy in (band_low, band_high, wo_core):
        copy.wait_send()
    for copy in spread_copies():
        if copy.is_remote:
            copy.wait_send()
    for copy in weight_copies():
        if copy.is_remote:
            copy.wait_send()

    @pl.loop(0, steps)
    def _(s):
        for copy in (
            to_x, to_y, pass_y, pass_x, corner_x, corner_y, sum_x, sum_y, wo_across, wo_pass
        ):
            copy(s).wait_send()

        @pl.when(far(s) == 0)
        def _():
            local_out(s).wait()

        @pl.when(far(s) != 0)
        def _():
            dispatch(s).wait_send()
            give_back(s).wait()


def apply_fused(ordered, spread, gate, up, down, queries, pairs, sinks, out_weight, out_gain):
    total, width = ordered.shape
    experts, _, units = gate.shape
    share = total // GROUPS
    rows = min(PART_ROWS, share)
    steps = total // rows
    hidden = 2 * experts * units
    sequence_rows, head_columns = queries.shape
    token_rows = sequence_rows // 4
    anywhere = pl.BlockSpec(memory_space=pl.ANY)
    vector = pl.BlockSpec(memory_space=pltpu.VMEM)
    scalar = pl.BlockSpec(memory_space=pltpu.SMEM)
    dma = pltpu.SemaphoreType.DMA
    return pl.pallas_call(
        functools.partial(fused_layer, steps, rows),
        out_shape=(
            jax.ShapeDtypeStruct((total, width), jnp.bfloat16),
            jax.ShapeDtypeStruct((token_rows, width), jnp.bfloat16),
        ),
        in_specs=[anywhere] * 7 + [scalar, anywhere, vector],
        out_specs=(anywhere, anywhere),
        scratch_shapes=[
            pltpu.VMEM((steps, QUAD * rows, width), jnp.bfloat16),
            pltpu.VMEM((GROUPS, QUAD) + spread.shape[-2:], jnp.float32),
            pltpu.VMEM((steps, QUAD * rows, EPG), jnp.float32),
            pltpu.VMEM((2 * experts, width, units), jnp.bfloat16),
            pltpu.VMEM((2 * experts, width, units), jnp.bfloat16),
            pltpu.VMEM((width, hidden), jnp.bfloat16),
            pltpu.VMEM((QUAD * rows, hidden), jnp.bfloat16),
            pltpu.VMEM((LAG, rows, width), jnp.float32),
            pltpu.VMEM((steps, (QUAD - 1) * rows, width), jnp.bfloat16),
            pltpu.VMEM((steps, rows, width), jnp.bfloat16),
            pltpu.VMEM((steps, 2 * rows, width), jnp.bfloat16),
            pltpu.VMEM((steps, rows, width), jnp.bfloat16),
            pltpu.VMEM(queries.shape, jnp.bfloat16),
            pltpu.VMEM((sequence_rows + 2 * WINDOW, pairs.shape[1]), jnp.bfloat16),
            pltpu.VMEM(queries.shape, jnp.bfloat16),
            pltpu.VMEM((3, token_rows, head_columns), jnp.bfloat16),
            pltpu.VMEM((4,) + out_weight.shape, jnp.bfloat16),
            pltpu.VMEM((token_rows, width), jnp.float32),
            pltpu.VMEM((token_rows, width), jnp.bfloat16),
            dma((steps, 10)),
            dma((steps, 10)),
            dma((3, 3 * experts)),
            dma((2, GROUPS * QUAD)),
            dma((3, 8)),
            dma((4, steps)),
        ],
        compiler_params=pltpu.CompilerParams(
            collective_id=0, has_side_effects=True, vmem_limit_bytes=66 * 10**6
        ),
        cost_estimate=pl.CostEstimate(
            flops=6 * QUAD * total * width * hidden,
            bytes_accessed=6 * experts * units * width,
            transcendentals=QUAD * total * hidden,
        ),
    )(ordered, spread, gate, up, down, queries, pairs, sinks, out_weight, out_gain)


def layer_fused(queries, key_rows, values, sink_logit, out_weight, out_gain, tokens, expert_ids,
                route_weight, gain, gate, up, down):
    token_total, width = tokens.shape
    share = token_total // GROUPS
    local_experts = gate.shape[0]
    inputs = tokens.astype(jnp.float32)
    normed = (
        inputs * lax.rsqrt(jnp.mean(inputs * inputs, axis=-1, keepdims=True) + epsilon) * gain
    ).astype(jnp.bfloat16)
    group = jnp.bitwise_xor(expert_ids[:, 0] // EPG, lax.axis_index("group"))
    in_group = (group[:, None] == jnp.arange(GROUPS, dtype=jnp.int32)).astype(jnp.float32)
    index = jnp.arange(token_total, dtype=jnp.int32)
    before = (index[None, :] < index[:, None]).astype(jnp.float32)
    ranks = jnp.dot(before, in_group, preferred_element_type=jnp.float32)
    rank = jnp.sum(ranks * in_group, axis=1).astype(jnp.int32)
    position = group * share + rank
    order = (position[None, :] == index[:, None]).astype(jnp.bfloat16)
    back = (position[:, None] == index[None, :]).astype(jnp.bfloat16)
    ordered = jnp.dot(order, normed, preferred_element_type=jnp.float32).astype(jnp.bfloat16)
    start = lax.axis_index("member") * local_experts
    member = (jnp.arange(EPG, dtype=jnp.int32) + start) % EPG
    spread = jnp.sum(
        jnp.where((expert_ids % EPG)[:, :, None] == member, route_weight[:, :, None], 0.0), axis=1
    )
    spread = jnp.dot(
        order.astype(jnp.float32), spread, precision=lax.Precision.HIGHEST,
        preferred_element_type=jnp.float32,
    )
    spread = spread.reshape(GROUPS, share, EPG).transpose(0, 2, 1)
    spread = jnp.stack([spread, jnp.roll(spread, local_experts, axis=1)])
    pairs = jnp.concatenate([key_rows, values, values, key_rows], axis=1)
    result, mixer_out = apply_fused(
        ordered, spread, gate, up, down, queries, pairs, sink_logit, out_weight,
        out_gain.reshape(1, width),
    )
    result = jnp.dot(back, result, preferred_element_type=jnp.float32).astype(jnp.bfloat16)
    return (mixer_out, result)


def can_fuse(queries, key_rows):
    return (
        lax.axis_size("group") == GROUPS
        and lax.axis_size("member") == 2
        and lax.axis_size("tp") == 4
        and key_rows.shape[1] == HEAD_DIM
        and queries.shape[1] % (2 * HEAD_DIM) == 0
    )


def local(queries, key_rows, values, sink_logit, out_weight, out_gain, routed_tokens,
          expert_ids, route_weight, routed_gain, expert_gate, expert_up, expert_down):
    if can_fuse(queries, key_rows):
        return layer_fused(
            queries, key_rows, values, sink_logit, out_weight, out_gain, routed_tokens,
            expert_ids, route_weight, routed_gain, expert_gate, expert_up, expert_down,
        )
    full_weight = lax.all_gather(out_weight, "tp", axis=0, tiled=True)
    attended = attention(queries, key_rows, values, sink_logit)
    experts_out, full_weight, attended = routed(
        routed_tokens, expert_ids, route_weight, routed_gain, expert_gate, expert_up, expert_down,
        full_weight, attended,
    )
    mixer_out = project(attended, full_weight, out_gain)
    return (mixer_out, experts_out)


def solution(mesh):
    ep, tp = mesh.shape["ep"], mesh.shape["tp"]
    split = Mesh(mesh.devices.reshape(GROUPS, ep // GROUPS, tp), ("group", "member", "tp"))
    every = ("group", "member", "tp")
    placed = (
        P(EP, "tp"),
        P(EP, "tp"),
        P(EP, "tp"),
        P("tp"),
        P("tp", None),
        P(),
        P(every, None),
        P(every, None),
        P(every, None),
        P(),
        P(EP, None, "tp"),
        P(EP, None, "tp"),
        P(EP, None, "tp"),
    )
    return jax.shard_map(
        local,
        mesh=split,
        in_specs=placed,
        out_specs=(P(every, None), P(every, None)),
        check_vma=False,
    )
```
